256 devices in a mesh: ep: 64 (over z, x, core), tp: 4 (over y).
Axes of the slice: x: 4, y: 4, z: 8, core: 2. Of those that a mesh axis runs over, the one named last changes fastest.
Arguments:
- query_rows: bfloat16 [12288, 1024], P('ep', 'tp'), may hold values from -8 to 8
- key_rows: bfloat16 [12288, 1024], P('ep', 'tp'), may hold values from -8 to 8
- value_rows: bfloat16 [12288, 1024], P('ep', 'tp'), may hold values from -6 to 6
- lambdas: float32 [8], P('tp'), may hold values from 0.3 to 0.8
- head_gain: float32 [128], replicated, may hold values from 0.1 to 1.9
- w_out: bfloat16 [1024, 2048], replicated, may hold values from -0.1875 to 0.1875
- moe_rows: bfloat16 [32768, 2048], P('ep'), may hold values from -6 to 6
- ffn_gain: float32 [2048], replicated, may hold values from 0.1 to 1.9
- routes: int32 [32768, 2], P('ep'), may hold values from 0 to 63, all different within a row; in each aligned block of 128 rows (0 to 127, 128 to 255, ...) at most 8 rows name the same one
- group_logits: float32 [32768, 4], P('ep'), may hold values from -8 to 8
- pick_logits: float32 [32768, 2], P('ep'), may hold values from -8 to 8
- w_gate: bfloat16 [64, 2048, 1024], P('ep', None, 'tp'), may hold values from -0.125 to 0.125
- w_up: bfloat16 [64, 2048, 1024], P('ep', None, 'tp'), may hold values from -0.125 to 0.125
- w_down: bfloat16 [64, 1024, 2048], P('ep', 'tp'), may hold values from -0.75 to 0.75
Outputs:
- mixer_out: bfloat16 [12288, 2048], P(('ep', 'tp'))
- moe_out: bfloat16 [32768, 2048], P(('ep', 'tp'))
The draws below stay inside these ranges and needn't reach their ends.
Inputs may be any that keep to these rules, and one draw needn't show every extreme that they name: `routes`: each row names 2 different experts. In each aligned block of 128 rows (the rows of one device) no expert is named by more than 8 rows; some expert is named by exactly 8 rows of a block.
All inputs are finite; a program needn't handle non-finite values.
Results may differ from the reference program's by a relative error of at most 0.015.
Values may be sent and summed in bfloat16 or wider, within the bound.
A program may use at most 128 MiB of HBM per device.

```python
import math
import jax
import jax.numpy as jnp
import numpy as np
from jax import lax

D = 2048
HEADS = 8
HEAD_QK = 64
HEAD_V = 128
FFE = 1024
GROUPS = 4
TOP = 2
TOKQ = 128
EXPERTS = 64
CAP = 8
TOKA = 12288
TOKB = 32768
N_EP = 64
N_TP = 4


def drawn_pair(key):
    base = jax.random.fold_in(key, 41)
    first, second = jax.random.split(base, 2)
    columns = HEADS * 2 * HEAD_QK
    queries = jnp.clip(jax.random.normal(first, (TOKA, columns), jnp.float32) * 1.3, -6.0, 6.0)
    keys = jnp.clip(jax.random.normal(second, (TOKA, columns), jnp.float32) * 1.3, -6.0, 6.0)
    return (queries, keys)


def draw_query_rows(key, part):
    return drawn_pair(key)[0].astype(jnp.bfloat16)


def draw_key_rows(key, part):
    return drawn_pair(key)[1].astype(jnp.bfloat16)


def steps_of(rng, extent, shards, least, largest):
    factor_of, own = 1.0, jax.random.fold_in(rng, 6)
    for axis_at, shards_of in shards:
        heights = jnp.exp(jax.random.uniform(jax.random.fold_in(own, axis_at), (shards_of,), jnp.float32, least / len(shards), largest / len(shards)))
        factor_of = factor_of * jnp.repeat(heights, extent[axis_at] // shards_of).reshape([-1 if axis == axis_at else 1 for axis in range(len(extent))])
    return factor_of


def routed_block(own_key, own, number, rows, count, top, reach, lean):
    order = jax.random.permutation(own_key, count)
    crowded, usual = shares(count, rows * top, reach, lean, True), shares(count, rows * top, reach, lean, False)
    places = jnp.arange(count)

    def named(sizes, offset_by):
        used = int((sizes > 0).sum())
        fixed = max(1, used // 4)
        moved = fixed + (places - fixed + offset_by * (used - fixed)) % max(1, count - fixed)
        return jnp.zeros((count,), jnp.int32).at[order[jnp.where(places < fixed, places, moved)]].set(jnp.asarray(sizes, jnp.int32))

    sizes = jnp.where(number % 4 == 0, named(crowded, number // 4), named(usual, number - number // 4 - 1))
    mixed = jax.random.permutation(jax.random.fold_in(own, 3), count)
    donor, taker = mixed[0:count // 2 * 2:2], mixed[1:count // 2 * 2:2]
    margin = jnp.minimum(sizes[donor] - 1, reach - sizes[taker]) // 2
    margin = jnp.where((donor == order[0]) | (taker == order[0]) | (sizes[taker] == 0), 0, jnp.maximum(margin, 0))
    moved = jax.random.randint(jax.random.fold_in(own, 4), (count // 2,), 0, 1 << 20) % (margin + 1)
    sizes = sizes.at[donor].add(-moved).at[taker].add(moved)
    members = jnp.searchsorted(jnp.cumsum(sizes), jnp.arange(rows * top), side="right").astype(jnp.int32)
    table = members.reshape(top, rows).T
    table = table[jax.random.permutation(jax.random.fold_in(own, 1), rows)]
    offset_by = jax.random.randint(jax.random.fold_in(own, 2), (rows, 1), 0, top)
    return jnp.take_along_axis(table, (jnp.arange(top)[None, :] + offset_by) % top, axis=1)


def shares(amount, total, bound, skew, full):
    weights = [(1 << 20) // math.isqrt(rank ** skew) + 1 for rank in range(1, amount + 1)]
    largest = bound if full else min(bound, max(-(-total // amount), total * weights[0] // sum(weights)))
    least = 1 if total - largest >= amount - 1 else 0
    given, rest = [largest] + [least] * (amount - 1), total - largest - least * (amount - 1)
    while rest > 0:
        movable = [i for i in range(1, amount) if given[i] < largest] or [i for i in range(1, amount) if given[i] < bound]
        pool, left = sum([weights[i] for i in movable]), rest
        for i in movable:
            addition = min(bound - given[i], max(1, left * weights[i] // pool), rest)
            given[i] = given[i] + addition
            rest = rest - addition
    return np.array(given)


def scatter_about(own_key, extent, width, most, cuts=(), kind=jnp.bfloat16):
    level = steps_of(own_key, extent, cuts, -0.22, 0.18) if cuts else 1.0
    drawn = jax.random.normal(own_key, extent, jnp.float32) * width * level
    return jnp.minimum(jnp.maximum(drawn, -most), most).astype(kind)


def setup_inputs(seed: int = 0) -> dict:
    key_list = jax.random.split(jax.random.key(seed), 15)
    query_rows = draw_query_rows(jax.random.fold_in(key_list[14], 71), 0)
    key_rows = draw_key_rows(jax.random.fold_in(key_list[14], 71), 0)
    value_rows = scatter_about(key_list[2], (TOKA, HEADS * HEAD_V), 1.0, 6.0, ((0, 64), (1, 4)))
    lambdas = jnp.clip(0.3 + 0.5 * jax.random.uniform(key_list[3], (HEADS,), jnp.float32) ** steps_of(key_list[3], (HEADS,), ((0, 4),), -0.2, 0.2), 0.3, 0.8)
    head_gain = jnp.clip(1.0 + 0.18 * jax.random.normal(key_list[4], (HEAD_V,), jnp.float32), 0.1, 1.9)
    w_out = scatter_about(key_list[5], (HEADS * HEAD_V, D), (HEADS * HEAD_V) ** -0.5, 0.1875)
    moe_rows = scatter_about(key_list[6], (TOKB, D), 1.0, 6.0, ((0, 64),))
    ffn_gain = jnp.clip(1.0 + 0.18 * jax.random.normal(key_list[7], (D,), jnp.float32), 0.1, 1.9)
    routes_keys = jax.random.split(jax.random.fold_in(key_list[8], 1), TOKB // TOKQ)
    routes_turns = jax.random.permutation(jax.random.fold_in(key_list[8], 3), TOKB // TOKQ)
    routes = jax.vmap(lambda own, number: routed_block(jax.random.fold_in(key_list[8], 2), own, number, TOKQ, EXPERTS, TOP, CAP, 1))(routes_keys, routes_turns).reshape((TOKB, TOP))
    group_logits = scatter_about(key_list[9], (TOKB, GROUPS), 2.0, 8.0, ((0, 64),), jnp.float32)
    pick_logits = scatter_about(key_list[10], (TOKB, TOP), 1.5, 8.0, ((0, 64),), jnp.float32)
    w_gate = scatter_about(key_list[11], (EXPERTS, D, FFE), D ** -0.5, 0.125, ((0, 64), (2, 4)))
    w_up = scatter_about(key_list[12], (EXPERTS, D, FFE), D ** -0.5, 0.125, ((0, 64), (2, 4)))
    w_down = scatter_about(key_list[13], (EXPERTS, FFE, D), (FFE // 16) ** -0.5, 0.75, ((0, 64), (1, 4)))
    return dict(query_rows=query_rows, key_rows=key_rows, value_rows=value_rows, lambdas=lambdas, head_gain=head_gain, w_out=w_out, moe_rows=moe_rows, ffn_gain=ffn_gain, routes=routes, group_logits=group_logits, pick_logits=pick_logits, w_gate=w_gate, w_up=w_up, w_down=w_down)


EPS = 1e-06
HEAD_SCALE = 0.8

def rms_rows(values, gain):
    squared = lax.optimization_barrier(jnp.mean(values * values, axis=-1, keepdims=True))
    return values * lax.rsqrt(squared + EPS) * gain

def attend(query_rows, key_rows, value_rows, lambdas, head_gain):
    token_count = query_rows.shape[0]
    block_rows = math.gcd(token_count, 128)
    keys = key_rows.astype(jnp.float32).reshape(token_count, HEADS, 2, HEAD_QK)
    values = value_rows.astype(jnp.float32).reshape(token_count, HEADS, HEAD_V)
    queries = query_rows.astype(jnp.float32).reshape(token_count // block_rows, block_rows, HEADS, 2, HEAD_QK)

    def one_block(query_block):
        scores = jnp.einsum('qhmd,khmd->hmqk', query_block, keys, precision=lax.Precision.HIGHEST) * HEAD_QK ** (-0.5)
        weights = jnp.exp(scores - lax.optimization_barrier(jnp.max(scores, axis=-1, keepdims=True)))
        totals = lax.optimization_barrier(jnp.sum(weights, axis=-1))
        rounded = lax.optimization_barrier(weights.astype(jnp.bfloat16)).astype(jnp.float32)
        sums = jnp.einsum('hmqk,khv->hmqv', rounded, values, precision=lax.Precision.HIGHEST)
        per_head = sums[:, 0] / totals[:, 0, :, None] - lambdas[:, None, None] * sums[:, 1] / totals[:, 1, :, None]
        normed = rms_rows(per_head, head_gain) * HEAD_SCALE
        return jnp.transpose(normed, (1, 0, 2)).reshape(block_rows, HEADS * HEAD_V).astype(jnp.bfloat16)
    return lax.map(one_block, queries).reshape(token_count, HEADS * HEAD_V)

def experts_part(moe_rows, ffn_gain, routes, group_logits, pick_logits, w_gate, w_up, w_down):
    model_width = moe_rows.shape[1]
    quarters = N_EP * N_TP
    normed = rms_rows(moe_rows.astype(jnp.float32), ffn_gain).astype(jnp.bfloat16)
    flattened = routes.reshape(quarters, TOKQ * TOP)
    onehot = (flattened[..., None] == jnp.arange(EXPERTS, dtype=jnp.int32)).astype(jnp.int32)
    before = jnp.cumsum(onehot, axis=1) - onehot
    ranking = lax.optimization_barrier(jnp.sum(before * onehot, axis=-1))
    slots = (flattened * quarters + jnp.arange(quarters, dtype=jnp.int32)[:, None]) * CAP + ranking
    source_rows = jnp.repeat(jnp.arange(TOKB, dtype=jnp.int32), TOP)
    buffer_rows = jnp.zeros((EXPERTS * quarters * CAP, model_width), jnp.bfloat16)
    buffer_rows = buffer_rows.at[slots.reshape(-1)].set(normed[source_rows])
    buffer_rows = buffer_rows.reshape(EXPERTS, quarters * CAP, model_width)
    unit_block = FFE // N_TP

    def run_expert(packed):
        expert_rows, gate_weight, up_weight, down_weight = packed
        gate_part = jnp.dot(expert_rows, gate_weight, preferred_element_type=jnp.float32)
        up_part = jnp.dot(expert_rows, up_weight, preferred_element_type=jnp.float32)
        hidden = (jax.nn.silu(gate_part) * up_part).astype(jnp.bfloat16)
        split_hidden = hidden.astype(jnp.float32).reshape(-1, N_TP, unit_block)
        split_down = down_weight.astype(jnp.float32).reshape(N_TP, unit_block, model_width)
        parts = jnp.einsum('rnf,nfd->nrd', split_hidden, split_down, precision=lax.Precision.HIGHEST)
        parts = lax.optimization_barrier(parts.astype(jnp.bfloat16)).astype(jnp.float32)
        return lax.optimization_barrier(jnp.sum(parts, axis=0)).astype(jnp.bfloat16)
    outputs = lax.map(run_expert, (buffer_rows, w_gate, w_up, w_down))
    picked = outputs.reshape(-1, model_width)[slots.reshape(-1)].reshape(TOKB, TOP, model_width)
    group_prob = jax.nn.softmax(group_logits, axis=-1)
    group_index = routes // (EXPERTS // GROUPS)
    matches = (group_index[..., None] == jnp.arange(GROUPS, dtype=jnp.int32)).astype(jnp.float32)
    group_share = lax.optimization_barrier(jnp.sum(group_prob[:, None, :] * matches, axis=-1))
    gate_values = group_share * jax.nn.softmax(pick_logits, axis=-1)
    return lax.optimization_barrier(jnp.sum(gate_values[..., None] * picked.astype(jnp.float32), axis=1)).astype(jnp.bfloat16)

def reference(query_rows, key_rows, value_rows, lambdas, head_gain, w_out, moe_rows, ffn_gain, routes, group_logits, pick_logits, w_gate, w_up, w_down):
    attended = attend(query_rows, key_rows, value_rows, lambdas, head_gain)
    mixer_out = jnp.dot(attended, w_out, preferred_element_type=jnp.float32).astype(jnp.bfloat16)
    moe_out = experts_part(moe_rows, ffn_gain, routes, group_logits, pick_logits, w_gate, w_up, w_down)
    return (mixer_out, moe_out)
```

```python
import functools

import jax
import jax.numpy as jnp
from jax import lax
from jax.experimental import pallas as pl
from jax.experimental.pallas import tpu as pltpu
from jax.sharding import PartitionSpec as P

EPS = 1e-06
HEAD_SCALE = 0.8
NZ, NX, NC, NY = 8, 4, 2, 4
ANY = pl.BlockSpec(memory_space=pl.ANY)
VMEM = pl.BlockSpec(memory_space=pltpu.VMEM)
MESH = pl.DeviceIdType.MESH


def rms_rows(values, gain):
    squared = jnp.mean(values * values, axis=-1, keepdims=True)
    return values * lax.rsqrt(squared + EPS) * gain


def plane_peer(ep, i):
    z, x, c = ep // (NX * NC), ep // NC % NX, ep % NC
    k, j = i % NZ, i // NZ
    dz = lax.rem(jnp.where(k % 2 == 1, (k + 1) // 2, NZ - k // 2), NZ)
    dx, dc = j // NC, j % NC
    return (lax.rem(z + dz, NZ) * NX + lax.rem(x + dx, NX)) * NC + lax.rem(c + dc, NC)


def gather_kernel(
    out_ref, g_ref, u_ref, d_ref, arrived_ref, gs_ref, us_ref, ds_ref, a_send, a_recv, w_send, w_recv, own_sem
):
    ep, tp = lax.axis_index("ep"), lax.axis_index("tp")
    right, left = lax.rem(tp + 1, NY), lax.rem(tp + NY - 1, NY)
    weights = ((g_ref, gs_ref), (u_ref, us_ref), (d_ref, ds_ref))

    def half(ref, h):
        rows = ref.shape[-2] // 2
        return ref.at[pl.ds(h * rows, rows)]

    def first(n, h, to_right):
        src, dst = weights[n]
        slot = 0 if to_right else 1
        at = (slot * 3 + n) * 2 + h
        return pltpu.make_async_remote_copy(
            src_ref=half(src, h),
            dst_ref=half(dst.at[slot], h),
            send_sem=w_send.at[at],
            recv_sem=w_recv.at[at],
            device_id=(ep, right if to_right else left),
            device_id_type=MESH,
        )

    def onward(n, to_right):
        src, dst = weights[n]
        slot, h = (0, 0) if to_right else (1, 1)
        at = 12 + slot * 3 + n
        return pltpu.make_async_remote_copy(
            src_ref=half(dst.at[slot], h),
            dst_ref=half(dst.at[2], h),
            send_sem=w_send.at[at],
            recv_sem=w_recv.at[at],
            device_id=(ep, right if to_right else left),
            device_id_type=MESH,
        )

    for turn in range(2):
        for n in range(3):
            first(n, turn, True).start()
            first(n, 1 - turn, False).start()

    def dispatch(i):
        peer = plane_peer(ep, i)
        return pltpu.make_async_remote_copy(
            src_ref=out_ref.at[peer],
            dst_ref=arrived_ref.at[ep],
            send_sem=a_send.at[i],
            recv_sem=a_recv.at[i],
            device_id=(peer, tp),
            device_id_type=MESH,
        )

    own = pltpu.make_async_copy(out_ref.at[ep], arrived_ref.at[ep], own_sem)
    own.start()

    def begin(i, carry):
        dispatch(i).start()
        return carry

    lax.fori_loop(1, NZ * NX * NC, begin, 0)
    for n in range(3):
        first(n, 0, True).wait_recv()
        onward(n, True).start()
        first(n, 1, False).wait_recv()
        onward(n, False).start()
    own.wait()

    def finish(i, carry):
        dispatch(i).wait()
        return carry

    lax.fori_loop(1, NZ * NX * NC, finish, 0)
    for n in range(3):
        first(n, 1, True).wait_recv()
        first(n, 0, False).wait_recv()
        for to_right in (True, False):
            first(n, 0, to_right).wait_send()
            first(n, 1, to_right).wait_send()
            onward(n, to_right).wait()


def gather_all(outgoing, w_gate, w_up, w_down):
    shape = lambda w: jax.ShapeDtypeStruct((3, *w.shape), w.dtype)
    peers = NZ * NX * NC
    return pl.pallas_call(
        gather_kernel,
        name="gather_all",
        out_shape=(jax.ShapeDtypeStruct(outgoing.shape, outgoing.dtype), shape(w_gate), shape(w_up), shape(w_down)),
        in_specs=[ANY] * 4,
        out_specs=(ANY,) * 4,
        scratch_shapes=[
            pltpu.SemaphoreType.DMA((peers,)),
            pltpu.SemaphoreType.DMA((peers,)),
            pltpu.SemaphoreType.DMA((18,)),
            pltpu.SemaphoreType.DMA((18,)),
            pltpu.SemaphoreType.DMA,
        ],
        compiler_params=pltpu.CompilerParams(has_side_effects=True),
        cost_estimate=pl.CostEstimate(flops=10**11, bytes_accessed=30 * 2**20, transcendentals=0),
    )(outgoing, w_gate, w_up, w_down)


def experts_kernel(x_ref, g_ref, u_ref, d_ref, gs_ref, us_ref, ds_ref, out_ref, total):
    def add(gate_weight, up_weight, down_weight, start):
        x = x_ref[...]
        gate = jnp.dot(x, gate_weight, preferred_element_type=jnp.float32)
        up = jnp.dot(x, up_weight, preferred_element_type=jnp.float32)
        hidden = (gate / (1.0 + jnp.exp(-gate)) * up).astype(jnp.bfloat16)
        part = jnp.dot(hidden, down_weight, preferred_element_type=jnp.float32)
        if start:
            total[...] = part
        else:
            total[...] += part

    step = pl.program_id(0)

    @pl.when(step == 0)
    def _():
        add(g_ref[...], u_ref[...], d_ref[...], True)

    @pl.when(step > 0)
    def _():
        add(gs_ref[0], us_ref[0], ds_ref[0], False)

    @pl.when(step == NY - 1)
    def _():
        out_ref[...] = total[...].astype(jnp.bfloat16)


def experts(rows, w_gate, w_up, w_down, gates, ups, downs):
    other = lambda w: pl.BlockSpec((1, *w.shape[1:]), lambda i: (jnp.maximum(i - 1, 0), 0, 0))
    whole = lambda w: pl.BlockSpec(w.shape, lambda i: (0, 0))
    return pl.pallas_call(
        experts_kernel,
        name="experts",
        grid=(NY,),
        out_shape=jax.ShapeDtypeStruct(rows.shape, jnp.bfloat16),
        in_specs=[whole(rows), whole(w_gate), whole(w_up), whole(w_down), other(gates), other(ups), other(downs)],
        out_specs=whole(rows),
        scratch_shapes=[pltpu.VMEM(rows.shape, jnp.float32)],
        compiler_params=pltpu.CompilerParams(
            dimension_semantics=("arbitrary",), vmem_limit_bytes=48 * 2**20
        ),
        cost_estimate=pl.CostEstimate(flops=6 * 10**9, bytes_accessed=16 * 2**20, transcendentals=0),
    )(rows, w_gate, w_up, w_down, gates, ups, downs)


def return_kernel(
    block,
    rows_ref, q_ref, kv_ref, lam_ref, gain_ref, returned_ref, heads_ref,
    kv, top, total, acc, done, a_send, a_recv, h_send, h_recv, own_sem,
):
    ep, tp = lax.axis_index("ep"), lax.axis_index("tp")
    chip, core = ep // NC, ep % NC
    head = tp * NC + core

    def give_back(i):
        peer = plane_peer(ep, i)
        return pltpu.make_async_remote_copy(
            src_ref=rows_ref.at[peer],
            dst_ref=returned_ref.at[ep],
            send_sem=a_send.at[i],
            recv_sem=a_recv.at[i],
            device_id=(peer, tp),
            device_id_type=MESH,
        )

    own = pltpu.make_async_copy(rows_ref.at[ep], returned_ref.at[ep], own_sem.at[0])
    load = pltpu.make_async_copy(kv_ref, kv, own_sem.at[1])
    own.start()
    load.start()

    def begin(i, carry):
        give_back(i).start()
        return carry

    lax.fori_loop(1, NZ * NX * NC, begin, 0)
    top[...] = jnp.full_like(top, -1e30)
    total[...] = jnp.zeros_like(total)
    acc[...] = jnp.zeros_like(acc)
    load.wait()

    def absorb(b, carry):
        rows = pl.ds(pl.multiple_of(b * block, block), block)
        keys = kv[rows, 0:128]
        scores = lax.dot_general(
            q_ref[...], keys, (((1,), (1,)), ((), ())), preferred_element_type=jnp.float32
        )
        old = top[...]
        new = jnp.maximum(old, jnp.max(scores, axis=-1, keepdims=True))
        factor = jnp.exp(old - new)
        weights = jnp.exp(scores - new)
        total[...] = total[...] * factor + jnp.sum(weights, axis=-1, keepdims=True)
        acc[...] = acc[...] * factor + jnp.dot(
            weights.astype(jnp.bfloat16), kv[rows, 128:256], preferred_element_type=jnp.float32
        )
        top[...] = new
        return carry

    lax.fori_loop(0, kv.shape[0] // block, absorb, 0)
    count = acc.shape[0] // 2
    per_head = acc[0:count] / total[0:count] - lam_ref[...] * (acc[count:] / total[count:])
    squared = jnp.mean(per_head * per_head, axis=-1, keepdims=True)
    normed = per_head * lax.rsqrt(squared + EPS) * gain_ref[...] * HEAD_SCALE
    done[...] = normed.astype(jnp.bfloat16).reshape(done.shape)

    def hand_on(i):
        to_core = lax.rem(core + i // NY, NC)
        to_tp = lax.rem(tp + i % NY, NY)
        return pltpu.make_async_remote_copy(
            src_ref=done.at[to_core * NY + to_tp],
            dst_ref=heads_ref.at[head],
            send_sem=h_send.at[i],
            recv_sem=h_recv.at[i],
            device_id=(chip * NC + to_core, to_tp),
            device_id_type=MESH,
        )

    keep = pltpu.make_async_copy(done.at[core * NY + tp], heads_ref.at[head], own_sem.at[2])
    keep.start()
    for i in range(1, NC * NY):
        hand_on(i).start()
    for i in range(1, NC * NY):
        hand_on(i).wait()
    keep.wait()
    own.wait()

    def finish(i, carry):
        give_back(i).wait()
        return carry

    lax.fori_loop(1, NZ * NX * NC, finish, 0)


def return_and_attend(rows, queries, keys_values, lam, gain):
    peers = NZ * NX * NC
    count = queries.shape[0]
    own_rows = count // 2 // (NC * NY)
    return pl.pallas_call(
        functools.partial(return_kernel, 1024),
        name="return_and_attend",
        out_shape=(
            jax.ShapeDtypeStruct(rows.shape, rows.dtype),
            jax.ShapeDtypeStruct((NC * NY, own_rows, 128), jnp.bfloat16),
        ),
        in_specs=[ANY, VMEM, ANY, VMEM, VMEM],
        out_specs=(ANY, ANY),
        scratch_shapes=[
            pltpu.VMEM(keys_values.shape, jnp.bfloat16),
            pltpu.VMEM((count, 1), jnp.float32),
            pltpu.VMEM((count, 1), jnp.float32),
            pltpu.VMEM((count, 128), jnp.float32),
            pltpu.VMEM((NC * NY, own_rows, 128), jnp.bfloat16),
            pltpu.SemaphoreType.DMA((peers,)),
            pltpu.SemaphoreType.DMA((peers,)),
            pltpu.SemaphoreType.DMA((NC * NY,)),
            pltpu.SemaphoreType.DMA((NC * NY,)),
            pltpu.SemaphoreType.DMA((3,)),
        ],
        compiler_params=pltpu.CompilerParams(has_side_effects=True, vmem_limit_bytes=56 * 2**20),
        cost_estimate=pl.CostEstimate(flops=4 * 10**9, bytes_accessed=16 * 2**20, transcendentals=0),
    )(rows, queries, keys_values, lam, gain)


def local(
    query_rows, key_rows, value_rows, lambdas, head_gain, w_out, moe_rows, ffn_gain,
    routes, group_logits, pick_logits, w_gate, w_up, w_down,
):
    ep, tp = lax.axis_index("ep"), lax.axis_index("tp")
    core = ep % NC
    peers = NZ * NX * NC

    rows_in = jnp.stack([query_rows, key_rows, value_rows])
    mine = lax.dynamic_slice_in_dim(rows_in, core * 128, 128, 2)
    other = lax.dynamic_slice_in_dim(rows_in, (1 - core) * 128, 128, 2)
    theirs = lax.ppermute(other, "ep", [(i, i ^ 1) for i in range(peers)])
    pair = jnp.where(core == 0, jnp.concatenate([mine, theirs], 1), jnp.concatenate([theirs, mine], 1))
    groups = [[i for i in range(peers) if i % NC == c] for c in range(NC)]
    keys_values = lax.all_gather(
        jnp.concatenate([pair[1], pair[2]], axis=1), "ep", axis=0, tiled=True, axis_index_groups=groups
    )
    scaled = pair[0] * jnp.bfloat16(0.125)
    zero = jnp.zeros((scaled.shape[0], 64), jnp.bfloat16)
    queries = jnp.concatenate(
        [jnp.concatenate([scaled[:, :64], zero], 1), jnp.concatenate([zero, scaled[:, 64:]], 1)], 0
    )

    quarter = moe_rows.shape[0] // NY
    top_k = routes.shape[1]
    capacity = 8
    own = lambda a: lax.dynamic_slice_in_dim(a, tp * quarter, quarter, 0)
    picks = own(routes)
    normed = rms_rows(own(moe_rows).astype(jnp.float32), ffn_gain).astype(jnp.bfloat16)
    flat = picks.reshape(-1)
    onehot = (flat[:, None] == jnp.arange(peers, dtype=jnp.int32)).astype(jnp.int32)
    ranking = jnp.sum((jnp.cumsum(onehot, axis=0) - onehot) * onehot, axis=-1)
    slots = (flat * capacity + ranking).reshape(quarter, top_k)
    at = slots[:, :, None] == jnp.arange(peers * capacity, dtype=jnp.int32)
    place = (at[:, 0] | at[:, 1]).astype(jnp.bfloat16)
    outgoing = lax.dot_general(
        place, normed, (((0,), (0,)), ((), ())), preferred_element_type=jnp.float32
    ).astype(jnp.bfloat16)

    arrived, gates, ups, downs = gather_all(
        outgoing.reshape(peers, capacity, -1), w_gate[0], w_up[0], w_down[0]
    )
    results = experts(arrived.reshape(peers * capacity, -1), w_gate[0], w_up[0], w_down[0], gates, ups, downs)
    returned, heads = return_and_attend(
        results.reshape(peers, capacity, -1),
        queries,
        keys_values,
        lax.dynamic_slice_in_dim(lambdas, core, 1, 0)[None],
        head_gain[None],
    )
    attended = jnp.transpose(heads, (1, 0, 2)).reshape(heads.shape[1], -1)
    mixer_out = jnp.dot(attended, w_out, preferred_element_type=jnp.float32).astype(jnp.bfloat16)

    group_count = group_logits.shape[1]
    group_prob = jax.nn.softmax(own(group_logits), axis=-1)
    matches = ((picks // (peers // group_count))[..., None] == jnp.arange(group_count, dtype=jnp.int32)).astype(
        jnp.float32
    )
    share = jnp.sum(group_prob[:, None, :] * matches, axis=-1)
    gate_values = share * jax.nn.softmax(own(pick_logits), axis=-1)
    mixing = jnp.sum(jnp.where(at, gate_values[:, :, None], 0.0), axis=1)
    high = mixing.astype(jnp.bfloat16)
    low = (mixing - high.astype(jnp.float32)).astype(jnp.bfloat16)
    back = returned.reshape(peers * capacity, -1)
    moe_out = (
        jnp.dot(high, back, preferred_element_type=jnp.float32)
        + jnp.dot(low, back, preferred_element_type=jnp.float32)
    ).astype(jnp.bfloat16)
    return mixer_out, moe_out


def solution(mesh):
    return jax.shard_map(
        local,
        mesh=mesh,
        in_specs=(
            P("ep", "tp"), P("ep", "tp"), P("ep", "tp"), P("tp"), P(), P(), P("ep", None), P(), P("ep", None),
            P("ep", None), P("ep", None), P("ep", None, "tp"), P("ep", None, "tp"), P("ep", "tp", None),
        ),
        out_specs=(P(("ep", "tp"), None), P(("ep", "tp"), None)),
        check_vma=False,
    )
```

```python
import functools

import jax
import jax.numpy as jnp
from jax import lax
from jax.experimental import pallas as pl
from jax.experimental.pallas import tpu as pltpu
from jax.sharding import PartitionSpec as P

EPS = 1e-06
HEAD_SCALE = 0.8
NZ, NX, NC, NY = 8, 4, 2, 4
ANY = pl.BlockSpec(memory_space=pl.ANY)
VMEM = pl.BlockSpec(memory_space=pltpu.VMEM)
MESH = pl.DeviceIdType.MESH


def plane_peer(ep, i):
    z, x, c = ep // (NX * NC), ep // NC % NX, ep % NC
    k, j = i % NZ, i // NZ
    dz = lax.rem(jnp.where(k % 2 == 1, (k + 1) // 2, NZ - k // 2), NZ)
    dx, dc = j // NC, j % NC
    return (lax.rem(z + dz, NZ) * NX + lax.rem(x + dx, NX)) * NC + lax.rem(c + dc, NC)


def step_kernel(
    parts, block,
    q_ref, k_ref, v_ref, lam_ref, gain_ref, w_out_ref, rows_ref, ffn_ref, place_ref, high_ref, low_ref,
    g_ref, u_ref, d_ref, mixer_ref, moe_ref,
    gates, ups, downs, sent, arrived, hidden, results, returned, queries, spread, kv, top, total, acc, done, heads, w_out,
    g_send, g_recv, d_send, d_recv, p_send, p_recv, z_send, z_recv, x_send, x_recv,
    a_send, a_recv, r_send, r_recv, h_send, h_recv, own_sem,
):
    ep, tp = lax.axis_index("ep"), lax.axis_index("tp")
    z, x, core = ep // (NX * NC), ep // NC % NX, ep % NC
    chip = ep // NC
    head = tp * NC + core
    peers = NZ * NX * NC
    f32 = jnp.float32

    def remote(src, dst, send, recv, at, device):
        return pltpu.make_async_remote_copy(
            src_ref=src, dst_ref=dst, send_sem=send.at[at], recv_sem=recv.at[at],
            device_id=device, device_id_type=MESH,
        )

    tp_side = (lax.rem(tp + 1, NY), lax.rem(tp + NY - 1, NY))

    def gate_up(n, step, side):
        src, full = ((g_ref, gates), (u_ref, ups))[n]
        rows = src.shape[0] // 2
        h = (step + side) % 2 if step < 2 else side
        part = pl.ds(h * rows, rows)
        frm = src.at[part] if step < 2 else full.at[1 + side, part]
        to = full.at[1 + side if step < 2 else 3, part]
        return remote(frm, to, g_send, g_recv, (n * 3 + step) * 2 + side, (ep, tp_side[side]))

    def down(j, step, side):
        cols = downs.shape[2]
        rows = d_ref.shape[0] // 2
        h = (step + side) % 2 if step < 2 else side
        row = lambda place: pl.ds((place * 2 + h) * rows, rows)
        if step < 2:
            frm = d_ref.at[pl.ds(h * rows, rows), pl.ds(j * cols, cols)]
            to = downs.at[j, row(1 + side)]
        else:
            frm = downs.at[j, row(1 + side)]
            to = downs.at[j, row(3)]
        return remote(frm, to, d_send, d_recv, (j * 3 + step) * 2 + side, (ep, tp_side[side]))

    both = lambda make: [make(0), make(1)]

    for step in range(2):
        for n in range(2):
            for c in both(lambda side: gate_up(n, step, side)):
                c.start()

    mine = pl.ds(pl.multiple_of(core * 128, 128), 128)
    other = pl.ds(pl.multiple_of((1 - core) * 128, 128), 128)
    count = q_ref.shape[0]
    place_of = pl.ds(pl.multiple_of(core * count, count), count)
    kv_rows = pl.ds(pl.multiple_of((chip * NC + core) * count, count), count)
    triples = (
        (q_ref, queries.at[place_of]),
        (k_ref, kv.at[kv_rows, pl.ds(0, 128)]),
        (v_ref, kv.at[kv_rows, pl.ds(128, 128)]),
    )
    partner = chip * NC + 1 - core
    swaps = [remote(src.at[:, other], dst, p_send, p_recv, n, (partner, tp)) for n, (src, dst) in enumerate(triples)]
    keeps = [pltpu.make_async_copy(src.at[:, mine], dst, own_sem.at[n]) for n, (src, dst) in enumerate(triples)]
    for c in swaps + keeps:
        c.start()
    deep = d_ref.shape[0]
    cols = downs.shape[2]
    loads = [
        pltpu.make_async_copy(g_ref, gates.at[0], own_sem.at[3]),
        pltpu.make_async_copy(u_ref, ups.at[0], own_sem.at[4]),
        pltpu.make_async_copy(w_out_ref, w_out, own_sem.at[5]),
    ] + [
        pltpu.make_async_copy(d_ref.at[:, pl.ds(j * cols, cols)], downs.at[j, pl.ds(0, deep)], own_sem.at[6 + j])
        for j in range(parts)
    ]
    for c in loads:
        c.start()

    chip_rows = kv.shape[0] // (NZ * NX)
    at_z = lambda dz: lax.rem(z + dz + NZ, NZ)
    at_x = lambda dx: lax.rem(x + dx + NX, NX)

    def kv_block(dz, dx, h=None):
        start = (at_z(dz) * NX + at_x(dx)) * chip_rows
        rows = chip_rows
        if h is not None:
            rows = chip_rows // 2
            start = start + h * rows
        return kv.at[pl.ds(pl.multiple_of(start, rows), rows)]

    def along_z(hop, side):
        sign = 1 if side == 0 else -1
        ref = kv_block(-sign * (hop - 1), 0, side if hop == NZ // 2 else None)
        device = ((at_z(sign) * NX + x) * NC + core, tp)
        return remote(ref, ref, z_send, z_recv, (hop - 1) * 2 + side, device)

    blocks = [0, -1, 1, -2, 2, -3, 3, 4]

    def along_x(b, step, side):
        sign = 1 if side == 0 else -1
        ref = kv_block(blocks[b], 0) if step == 0 else kv_block(blocks[b], -sign, side)
        device = ((z * NX + at_x(sign)) * NC + core, tp)
        return remote(ref, ref, x_send, x_recv, (b * 2 + step) * 2 + side, device)

    def x_first(b):
        for c in both(lambda side: along_x(b, 0, side)):
            c.start()

    def x_onward(b):
        for side in range(2):
            along_x(b, 0, side).wait_recv()
            along_x(b, 1, side).start()

    def z_hop(hop):
        for side in range(2):
            along_z(hop, side).wait_recv()
            if hop < NZ // 2:
                along_z(hop + 1, side).start()

    def dispatch(i):
        peer = plane_peer(ep, i)
        return remote(sent.at[peer], arrived.at[ep], a_send, a_recv, i, (peer, tp))

    def give_back(j, i):
        peer = plane_peer(ep, i)
        return remote(results.at[j, peer], returned.at[j, ep], r_send, r_recv, j * peers + i, (peer, tp))

    def each(first, last, act):
        def one(i, carry):
            act(i)
            return carry

        lax.fori_loop(first, last, one, 0)

    rows = rows_ref[...].astype(f32)
    squared = jnp.mean(rows * rows, axis=-1, keepdims=True)
    normed = (rows * lax.rsqrt(squared + EPS) * ffn_ref[...]).astype(jnp.bfloat16)
    sent[...] = jnp.dot(place_ref[...], normed, preferred_element_type=f32).astype(jnp.bfloat16).reshape(sent.shape)

    for c in keeps:
        c.wait()
    for c in swaps:
        c.wait()
    for c in both(lambda side: along_z(1, side)):
        c.start()
    x_first(0)
    each(1, 22, lambda i: dispatch(i).start())
    z_hop(1)
    x_first(1)
    x_first(2)
    each(22, 43, lambda i: dispatch(i).start())
    for side in range(2):
        gate_up(0, 0, side).wait_recv()
        gate_up(0, 2, side).start()
    z_hop(2)
    x_onward(0)
    x_first(3)
    x_first(4)
    each(43, 64, lambda i: dispatch(i).start())
    arrived[ep] = sent[ep]
    for side in range(2):
        gate_up(1, 0, side).wait_recv()
        gate_up(1, 2, side).start()
    for step in range(2):
        for c in both(lambda side: down(0, step, side)):
            c.start()
    for b in (1, 2):
        x_onward(b)
    z_hop(3)
    x_first(5)
    x_first(6)
    for b in (3, 4):
        x_onward(b)
    z_hop(4)
    x_first(7)

    scaled = queries[...] * jnp.bfloat16(0.125)
    column = lax.broadcasted_iota(jnp.int32, scaled.shape, 1)
    zero = jnp.zeros_like(scaled)
    spread[0 : 2 * count] = jnp.where(column < 64, scaled, zero)
    spread[2 * count :] = jnp.where(column < 64, zero, scaled)
    top[...] = jnp.full_like(top, -1e30)
    total[...] = jnp.zeros_like(total)
    acc[...] = jnp.zeros_like(acc)

    each(1, peers, lambda i: dispatch(i).wait_recv())
    for c in loads[:2]:
        c.wait()

    def one_part(s, carry):
        @pl.when(s == 1)
        def _():
            for n in range(2):
                gate_up(n, 1, 0).wait_recv()
            for b in (5, 6):
                x_onward(b)

        @pl.when(s == 2)
        def _():
            for n in range(2):
                gate_up(n, 1, 1).wait_recv()
            x_onward(7)

        @pl.when(s == 3)
        def _():
            for n in range(2):
                for side in range(2):
                    gate_up(n, 2, side).wait_recv()

        rows_in = arrived[...].reshape(peers * arrived.shape[1], arrived.shape[2])
        gate = jnp.dot(rows_in, gates[s], preferred_element_type=f32)
        up = jnp.dot(rows_in, ups[s], preferred_element_type=f32)
        hidden[:, pl.ds(pl.multiple_of(s * deep, deep), deep)] = (gate / (1.0 + jnp.exp(-gate)) * up).astype(jnp.bfloat16)
        return carry

    lax.fori_loop(0, NY, one_part, 0)

    def absorb(b, carry):
        at = pl.ds(pl.multiple_of(b * block, block), block)
        scores = lax.dot_general(spread[...], kv[at, 0:128], (((1,), (1,)), ((), ())), preferred_element_type=f32)
        old = top[...]
        new = jnp.maximum(old, jnp.max(scores, axis=-1, keepdims=True))
        factor = jnp.exp(old - new)
        weights = jnp.exp(scores - new)
        total[...] = total[...] * factor + jnp.sum(weights, axis=-1, keepdims=True)
        acc[...] = acc[...] * factor + jnp.dot(
            weights.astype(jnp.bfloat16), kv[at, 128:256], preferred_element_type=f32
        )
        top[...] = new
        return carry

    turns = kv.shape[0] // block

    def one_chunk(j, carry):
        for k in range(parts):
            @pl.when(j == k)
            def _(k=k):
                for side in range(2):
                    down(k, 0, side).wait_recv()
                    down(k, 2, side).start()
                if k + 1 < parts:
                    for step in range(2):
                        for c in both(lambda side: down(k + 1, step, side)):
                            c.start()
                loads[3 + k].wait()
                if k == 1:
                    for b in range(NZ):
                        for side in range(2):
                            along_x(b, 1, side).wait_recv()

        @pl.when(j > 0)
        def _():
            lax.fori_loop((j - 1) * turns // (parts - 1), j * turns // (parts - 1), absorb, 0)

        for k in range(parts):
            @pl.when(j == k)
            def _(k=k):
                for side in range(2):
                    down(k, 1, side).wait_recv()
                    down(k, 2, side).wait_recv()

        results[j] = (
            jnp.dot(hidden[...], downs[j], preferred_element_type=f32).astype(jnp.bfloat16).reshape(results.shape[1:])
        )
        returned[j, ep] = results[j, ep]
        each(1, peers, lambda i: give_back(j, i).start())
        return carry

    lax.fori_loop(0, parts, one_chunk, 0)

    per_head = acc[0 : 2 * count] / total[0 : 2 * count] - lam_ref[...] * (acc[2 * count :] / total[2 * count :])
    squared = jnp.mean(per_head * per_head, axis=-1, keepdims=True)
    normed = per_head * lax.rsqrt(squared + EPS) * gain_ref[...] * HEAD_SCALE
    done[...] = normed.astype(jnp.bfloat16).reshape(done.shape)

    def hand_on(i):
        to_core = lax.rem(core + i // NY, NC)
        to_tp = lax.rem(tp + i % NY, NY)
        return remote(
            done.at[to_core * NY + to_tp], heads.at[head], h_send, h_recv, i, (chip * NC + to_core, to_tp)
        )

    for i in range(1, NC * NY):
        hand_on(i).start()
    heads[head] = done[core * NY + tp]
    for i in range(1, NC * NY):
        hand_on(i).wait()
    loads[2].wait()
    attended = jnp.concatenate([heads[i] for i in range(NC * NY)], axis=1)
    mixer_ref[...] = jnp.dot(attended, w_out[...], preferred_element_type=f32).astype(jnp.bfloat16)

    def combine(j, carry):
        each(1, peers, lambda i: give_back(j, i).wait_recv())
        back = returned[j].reshape(peers * returned.shape[2], cols)
        moe_ref[:, pl.ds(pl.multiple_of(j * cols, cols), cols)] = (
            jnp.dot(high_ref[...], back, preferred_element_type=f32)
            + jnp.dot(low_ref[...], back, preferred_element_type=f32)
        ).astype(jnp.bfloat16)
        return carry

    lax.fori_loop(0, parts, combine, 0)

    each(1, peers, lambda i: dispatch(i).wait_send())
    for j in range(parts):
        each(1, peers, lambda i: give_back(j, i).wait_send())
    for side in range(2):
        for step in range(3):
            for n in range(2):
                gate_up(n, step, side).wait_send()
            for j in range(parts):
                down(j, step, side).wait_send()
        for hop in range(1, NZ // 2 + 1):
            along_z(hop, side).wait_send()
        for b in range(NZ):
            for step in range(2):
                along_x(b, step, side).wait_send()


def whole_step(parts, block, *args):
    q, k, v, lam, gain, w_out, rows, ffn, place, high, low, w_gate, w_up, w_down = args
    bf16, f32 = jnp.bfloat16, jnp.float32
    peers = NZ * NX * NC
    count, width = q.shape[0], rows.shape[1]
    capacity = place.shape[0] // peers
    deep = w_down.shape[0]
    own_rows = count // NY
    dma = lambda n: pltpu.SemaphoreType.DMA((n,))
    return pl.pallas_call(
        functools.partial(step_kernel, parts, block),
        name="whole_step",
        out_shape=(
            jax.ShapeDtypeStruct((own_rows, width), bf16),
            jax.ShapeDtypeStruct((rows.shape[0], width), bf16),
        ),
        in_specs=[ANY, ANY, ANY, VMEM, VMEM, ANY, VMEM, VMEM, VMEM, VMEM, VMEM, ANY, ANY, ANY],
        out_specs=(VMEM, VMEM),
        scratch_shapes=[
            pltpu.VMEM((NY, *w_gate.shape), bf16),
            pltpu.VMEM((NY, *w_up.shape), bf16),
            pltpu.VMEM((parts, NY * deep, width // parts), bf16),
            pltpu.VMEM((peers, capacity, width), bf16),
            pltpu.VMEM((peers, capacity, width), bf16),
            pltpu.VMEM((peers * capacity, NY * deep), bf16),
            pltpu.VMEM((parts, peers, capacity, width // parts), bf16),
            pltpu.VMEM((parts, peers, capacity, width // parts), bf16),
            pltpu.VMEM((2 * count, 128), bf16),
            pltpu.VMEM((4 * count, 128), bf16),
            pltpu.VMEM((peers * count, 256), bf16),
            pltpu.VMEM((4 * count, 1), f32),
            pltpu.VMEM((4 * count, 1), f32),
            pltpu.VMEM((4 * count, 128), f32),
            pltpu.VMEM((NC * NY, own_rows, 128), bf16),
            pltpu.VMEM((NC * NY, own_rows, 128), bf16),
            pltpu.VMEM(w_out.shape, bf16),
            dma(12), dma(12), dma(6 * parts), dma(6 * parts), dma(3), dma(3), dma(NZ), dma(NZ), dma(4 * NZ), dma(4 * NZ),
            dma(peers), dma(peers), dma(parts * peers), dma(parts * peers), dma(NC * NY), dma(NC * NY), dma(6 + parts),
        ],
        compiler_params=pltpu.CompilerParams(has_side_effects=True, vmem_limit_bytes=60 * 2**20),
        cost_estimate=pl.CostEstimate(flops=10**10, bytes_accessed=16 * 2**20, transcendentals=0),
    )(*args)


def local(
    query_rows, key_rows, value_rows, lambdas, head_gain, w_out, moe_rows, ffn_gain,
    routes, group_logits, pick_logits, w_gate, w_up, w_down,
):
    ep, tp = lax.axis_index("ep"), lax.axis_index("tp")
    core = ep % NC
    peers = NZ * NX * NC
    quarter = moe_rows.shape[0] // NY
    top_k = routes.shape[1]
    capacity = 8
    own = lambda a: lax.dynamic_slice_in_dim(a, tp * quarter, quarter, 0)
    picks = own(routes)
    flat = picks.reshape(-1)
    onehot = (flat[:, None] == jnp.arange(peers, dtype=jnp.int32)).astype(jnp.int32)
    ranking = jnp.sum((jnp.cumsum(onehot, axis=0) - onehot) * onehot, axis=-1)
    slots = (flat * capacity + ranking).reshape(quarter, top_k)
    every = jnp.arange(peers * capacity, dtype=jnp.int32)
    place = ((slots[None, :, 0] == every[:, None]) | (slots[None, :, 1] == every[:, None])).astype(jnp.bfloat16)
    group_count = group_logits.shape[1]
    group_prob = jax.nn.softmax(own(group_logits), axis=-1)
    matches = ((picks // (peers // group_count))[..., None] == jnp.arange(group_count, dtype=jnp.int32)).astype(
        jnp.float32
    )
    share = jnp.sum(group_prob[:, None, :] * matches, axis=-1)
    gate_values = share * jax.nn.softmax(own(pick_logits), axis=-1)
    mixing = jnp.sum(jnp.where(slots[:, :, None] == every, gate_values[:, :, None], 0.0), axis=1)
    high = mixing.astype(jnp.bfloat16)
    low = (mixing - high.astype(jnp.float32)).astype(jnp.bfloat16)
    return whole_step(
        4, 1024,
        query_rows, key_rows, value_rows, lax.dynamic_slice_in_dim(lambdas, core, 1, 0)[None], head_gain[None], w_out,
        own(moe_rows), ffn_gain[None], place, high, low, w_gate[0], w_up[0], w_down[0],
    )


def solution(mesh):
    return jax.shard_map(
        local,
        mesh=mesh,
        in_specs=(
            P("ep", "tp"), P("ep", "tp"), P("ep", "tp"), P("tp"), P(), P(), P("ep", None), P(), P("ep", None),
            P("ep", None), P("ep", None), P("ep", None, "tp"), P("ep", None, "tp"), P("ep", "tp", None),
        ),
        out_specs=(P(("ep", "tp"), None), P(("ep", "tp"), None)),
        check_vma=False,
    )
```

```python
import functools

import jax
import jax.numpy as jnp
from jax import lax
from jax.experimental import pallas as pl
from jax.experimental.pallas import tpu as pltpu
from jax.sharding import PartitionSpec as P

EPS = 1e-06
HEAD_SCALE = 0.8
NZ, NX, NC, NY = 8, 4, 2, 4
ANY = pl.BlockSpec(memory_space=pl.ANY)
VMEM = pl.BlockSpec(memory_space=pltpu.VMEM)
MESH = pl.DeviceIdType.MESH


def plane_peer(ep, i):
    z, x, c = ep // (NX * NC), ep // NC % NX, ep % NC
    k, j = i % NZ, i // NZ
    dz = lax.rem(jnp.where(k % 2 == 1, (k + 1) // 2, NZ - k // 2), NZ)
    dx, dc = j // NC, j % NC
    return (lax.rem(z + dz, NZ) * NX + lax.rem(x + dx, NX)) * NC + lax.rem(c + dc, NC)


def step_kernel(
    parts,
    q_ref, k_ref, v_ref, lam_ref, gain_ref, w_out_ref, rows_ref, ffn_ref, routes_ref, groups_ref, picks_ref,
    g_ref, u_ref, d_ref, mixer_ref, moe_ref,
    rows_in, high, low, gates, ups, downs, sent, arrived, hidden, results, returned, queries, spread, kv, top, total, acc, done, heads, w_out,
    g_send, g_recv, d_send, d_recv, p_send, p_recv, z_send, z_recv, x_send, x_recv,
    a_send, a_recv, r_send, r_recv, h_send, h_recv, own_sem,
):
    ep, tp = lax.axis_index("ep"), lax.axis_index("tp")
    z, x, core = ep // (NX * NC), ep // NC % NX, ep % NC
    chip = ep // NC
    head = tp * NC + core
    peers = NZ * NX * NC
    f32 = jnp.float32

    def remote(src, dst, send, recv, at, device):
        return pltpu.make_async_remote_copy(
            src_ref=src, dst_ref=dst, send_sem=send.at[at], recv_sem=recv.at[at],
            device_id=device, device_id_type=MESH,
        )

    tp_side = (lax.rem(tp + 1, NY), lax.rem(tp + NY - 1, NY))

    def gate_up(n, step, side):
        src, full = ((g_ref, gates), (u_ref, ups))[n]
        rows = src.shape[0] // 2
        h = (step + side) % 2 if step < 2 else side
        part = pl.ds(h * rows, rows)
        frm = src.at[part] if step < 2 else full.at[1 + side, part]
        to = full.at[1 + side if step < 2 else 3, part]
        return remote(frm, to, g_send, g_recv, (n * 3 + step) * 2 + side, (ep, tp_side[side]))

    def down(j, step, side):
        cols = downs.shape[2]
        rows = d_ref.shape[0] // 2
        h = (step + side) % 2 if step < 2 else side
        row = lambda place: pl.ds((place * 2 + h) * rows, rows)
        if step < 2:
            frm = d_ref.at[pl.ds(h * rows, rows), pl.ds(j * cols, cols)]
            to = downs.at[j, row(1 + side)]
        else:
            frm = downs.at[j, row(1 + side)]
            to = downs.at[j, row(3)]
        return remote(frm, to, d_send, d_recv, (j * 3 + step) * 2 + side, (ep, tp_side[side]))

    both = lambda make: [make(0), make(1)]

    for step in range(2):
        for n in range(2):
            for c in both(lambda side: gate_up(n, step, side)):
                c.start()

    mine = pl.ds(pl.multiple_of(core * 128, 128), 128)
    other = pl.ds(pl.multiple_of((1 - core) * 128, 128), 128)
    count = q_ref.shape[0]
    place_of = pl.ds(pl.multiple_of(core * count, count), count)
    kv_rows = pl.ds(pl.multiple_of((chip * NC + core) * count, count), count)
    triples = (
        (q_ref, queries.at[place_of]),
        (k_ref, kv.at[kv_rows, pl.ds(0, 128)]),
        (v_ref, kv.at[kv_rows, pl.ds(128, 128)]),
    )
    partner = chip * NC + 1 - core
    swaps = [remote(src.at[:, other], dst, p_send, p_recv, n, (partner, tp)) for n, (src, dst) in enumerate(triples)]
    keeps = [pltpu.make_async_copy(src.at[:, mine], dst, own_sem.at[n]) for n, (src, dst) in enumerate(triples)]
    for c in swaps + keeps:
        c.start()
    deep = d_ref.shape[0]
    cols = downs.shape[2]
    loads = [
        pltpu.make_async_copy(g_ref, gates.at[0], own_sem.at[3]),
        pltpu.make_async_copy(u_ref, ups.at[0], own_sem.at[4]),
        pltpu.make_async_copy(w_out_ref, w_out, own_sem.at[5]),
    ] + [
        pltpu.make_async_copy(d_ref.at[:, pl.ds(j * cols, cols)], downs.at[j, pl.ds(0, deep)], own_sem.at[6 + j])
        for j in range(parts)
    ]
    tokens = rows_in.shape[0]
    load_rows = pltpu.make_async_copy(
        rows_ref.at[pl.ds(pl.multiple_of(tp * tokens, tokens), tokens)], rows_in, own_sem.at[6 + parts]
    )
    for c in [load_rows] + loads:
        c.start()

    chip_rows = kv.shape[0] // (NZ * NX)
    at_z = lambda dz: lax.rem(z + dz + NZ, NZ)
    at_x = lambda dx: lax.rem(x + dx + NX, NX)

    def kv_block(dz, dx, h=None):
        start = (at_z(dz) * NX + at_x(dx)) * chip_rows
        rows = chip_rows
        if h is not None:
            rows = chip_rows // 2
            start = start + h * rows
        return kv.at[pl.ds(pl.multiple_of(start, rows), rows)]

    def along_z(hop, side):
        sign = 1 if side == 0 else -1
        ref = kv_block(-sign * (hop - 1), 0, side if hop == NZ // 2 else None)
        device = ((at_z(sign) * NX + x) * NC + core, tp)
        return remote(ref, ref, z_send, z_recv, (hop - 1) * 2 + side, device)

    blocks = [0, -1, 1, -2, 2, -3, 3, 4]

    def along_x(b, step, side):
        sign = 1 if side == 0 else -1
        ref = kv_block(blocks[b], 0) if step == 0 else kv_block(blocks[b], -sign, side)
        device = ((z * NX + at_x(sign)) * NC + core, tp)
        return remote(ref, ref, x_send, x_recv, (b * 2 + step) * 2 + side, device)

    def x_first(b):
        for c in both(lambda side: along_x(b, 0, side)):
            c.start()

    def x_onward(b):
        for side in range(2):
            along_x(b, 0, side).wait_recv()
            along_x(b, 1, side).start()

    def z_hop(hop):
        for side in range(2):
            along_z(hop, side).wait_recv()
            if hop < NZ // 2:
                along_z(hop + 1, side).start()

    def dispatch(i):
        peer = plane_peer(ep, i)
        return remote(sent.at[peer], arrived.at[ep], a_send, a_recv, i, (peer, tp))

    def give_back(j, i):
        peer = plane_peer(ep, i)
        return remote(results.at[j, peer], returned.at[j, ep], r_send, r_recv, j * peers + i, (peer, tp))

    def each(first, last, act):
        def one(i, carry):
            act(i)
            return carry

        lax.fori_loop(first, last, one, 0)

    load_rows.wait()
    rows = rows_in[...].astype(f32)
    squared = jnp.mean(rows * rows, axis=-1, keepdims=True)
    normed = (rows * lax.rsqrt(squared + EPS) * ffn_ref[...]).astype(jnp.bfloat16)
    own_rows = pl.ds(pl.multiple_of(tp * tokens, tokens), tokens)
    chosen = routes_ref[own_rows, :]
    logits = groups_ref[own_rows, :]
    group_weights = jnp.exp(logits - jnp.max(logits, axis=-1, keepdims=True))
    group_weights = group_weights / jnp.sum(group_weights, axis=-1, keepdims=True)
    logits = picks_ref[own_rows, :]
    pick_weights = jnp.exp(logits - jnp.max(logits, axis=-1, keepdims=True))
    pick_weights = pick_weights / jnp.sum(pick_weights, axis=-1, keepdims=True)
    lane = lax.broadcasted_iota(jnp.int32, (tokens, tokens), 1)
    earlier = (lane < lax.broadcasted_iota(jnp.int32, (tokens, tokens), 0)).astype(f32).astype(jnp.bfloat16)
    named = [lane == chosen[:, k : k + 1] for k in range(2)]
    either = jnp.where(named[0] | named[1], 1.0, 0.0).astype(jnp.bfloat16)
    before = jnp.dot(earlier, either, preferred_element_type=f32)
    capacity = sent.shape[1]
    every = lax.broadcasted_iota(jnp.int32, (tokens, peers * capacity), 1).astype(f32)
    group_size = peers // groups_ref.shape[1]
    group_lane = lax.broadcasted_iota(jnp.int32, group_weights.shape, 1) * group_size
    place = jnp.zeros((tokens, peers * capacity), f32)
    mixing = jnp.zeros((tokens, peers * capacity), f32)
    for k in range(2):
        expert = chosen[:, k : k + 1]
        rank = jnp.sum(jnp.where(named[k], before, 0.0), axis=-1, keepdims=True)
        hit = every == expert.astype(f32) * capacity + rank
        inside = (expert >= group_lane) & (expert < group_lane + group_size)
        share = jnp.sum(jnp.where(inside, group_weights, 0.0), axis=-1, keepdims=True)
        place = jnp.where(hit, 1.0, place)
        mixing = jnp.where(hit, share * pick_weights[:, k : k + 1], mixing)
    high[...] = mixing.astype(jnp.bfloat16)
    low[...] = (mixing - mixing.astype(jnp.bfloat16).astype(f32)).astype(jnp.bfloat16)
    sent[...] = (
        lax.dot_general(place.astype(jnp.bfloat16), normed, (((0,), (0,)), ((), ())), preferred_element_type=f32)
        .astype(jnp.bfloat16)
        .reshape(sent.shape)
    )
    arrived[ep] = sent[ep]

    for c in keeps:
        c.wait()
    for c in swaps:
        c.wait()
    for c in both(lambda side: along_z(1, side)):
        c.start()
    x_first(0)
    each(1, peers, lambda i: dispatch(i).start())

    scaled = queries[...] * jnp.bfloat16(0.125)
    column = lax.broadcasted_iota(jnp.int32, scaled.shape, 1)
    zero = jnp.zeros_like(scaled)
    spread[0 : 2 * count] = jnp.where(column < 64, scaled, zero)
    spread[2 * count :] = jnp.where(column < 64, zero, scaled)
    top[...] = jnp.full_like(top, -1e30)
    total[...] = jnp.zeros_like(total)
    acc[...] = jnp.zeros_like(acc)

    z_hop(1)
    x_first(1)
    x_first(2)
    for n in range(2):
        for side in range(2):
            gate_up(n, 0, side).wait_recv()
            gate_up(n, 2, side).start()
    for j in range(2):
        for step in range(2):
            for c in both(lambda side: down(j, step, side)):
                c.start()
    x_onward(0)
    for b in (1, 2):
        x_onward(b)

    def absorb(b):
        for side in range(2):
            along_x(b, 1, side).wait_recv()
        size = NX * chip_rows
        at = pl.ds(pl.multiple_of(at_z(blocks[b]) * size, size), size)
        absorb_at(at)

    def absorb_at(at):
        scores = lax.dot_general(spread[...], kv[at, 0:128], (((1,), (1,)), ((), ())), preferred_element_type=f32)
        old = top[...]
        new = jnp.maximum(old, jnp.max(scores, axis=-1, keepdims=True))
        factor = jnp.exp(old - new)
        weights = jnp.exp(scores - new)
        total[...] = total[...] * factor + jnp.sum(weights, axis=-1, keepdims=True)
        acc[...] = acc[...] * factor + jnp.dot(
            weights.astype(jnp.bfloat16), kv[at, 128:256], preferred_element_type=f32
        )
        top[...] = new

    for b in range(3):
        absorb(b)

    each(1, peers, lambda i: dispatch(i).wait_recv())
    for c in loads[:2]:
        c.wait()

    def one_part(s, carry):
        @pl.when(s == 1)
        def _():
            for n in range(2):
                gate_up(n, 1, 0).wait_recv()
            z_hop(2)
            x_first(3)
            x_first(4)

        @pl.when(s == 2)
        def _():
            for n in range(2):
                gate_up(n, 1, 1).wait_recv()

        @pl.when(s == 3)
        def _():
            for n in range(2):
                for side in range(2):
                    gate_up(n, 2, side).wait_recv()

        rows_at = arrived[...].reshape(peers * arrived.shape[1], arrived.shape[2])
        gate = jnp.dot(rows_at, gates[s], preferred_element_type=f32)
        up = jnp.dot(rows_at, ups[s], preferred_element_type=f32)
        hidden[:, pl.ds(pl.multiple_of(s * deep, deep), deep)] = (gate / (1.0 + jnp.exp(-gate)) * up).astype(jnp.bfloat16)
        return carry

    lax.fori_loop(0, NY, one_part, 0)

    def down_onward(j):
        for side in range(2):
            down(j, 0, side).wait_recv()
            down(j, 2, side).start()
        if j + 2 < parts:
            for step in range(2):
                for c in both(lambda side: down(j + 2, step, side)):
                    c.start()

    def between(j):
        if j == 0:
            down_onward(0)
            z_hop(3)
            x_first(5)
            x_first(6)
            down_onward(1)
            x_onward(3)
            x_onward(4)
            z_hop(4)
            x_first(7)
        elif j == 1:
            down_onward(2)
            x_onward(5)
            x_onward(6)
            absorb(3)
            absorb(4)
        elif j == 2:
            down_onward(3)
            x_onward(7)
            absorb(5)

    def one_chunk(j, carry):
        for k in range(parts):
            @pl.when(j == k)
            def _(k=k):
                between(k)
                for side in range(2):
                    down(k, 1, side).wait_recv()
                    down(k, 2, side).wait_recv()
                loads[3 + k].wait()

        results[j] = (
            jnp.dot(hidden[...], downs[j], preferred_element_type=f32).astype(jnp.bfloat16).reshape(results.shape[1:])
        )
        returned[j, ep] = results[j, ep]
        each(1, peers, lambda i: give_back(j, i).start())
        return carry

    lax.fori_loop(0, parts, one_chunk, 0)
    absorb(6)
    absorb(7)

    per_head = acc[0 : 2 * count] / total[0 : 2 * count] - lam_ref[...] * (acc[2 * count :] / total[2 * count :])
    squared = jnp.mean(per_head * per_head, axis=-1, keepdims=True)
    normed = per_head * lax.rsqrt(squared + EPS) * gain_ref[...] * HEAD_SCALE
    done[...] = normed.astype(jnp.bfloat16).reshape(done.shape)

    def hand_on(i):
        to_core = lax.rem(core + i // NY, NC)
        to_tp = lax.rem(tp + i % NY, NY)
        return remote(
            done.at[to_core * NY + to_tp], heads.at[head], h_send, h_recv, i, (chip * NC + to_core, to_tp)
        )

    for i in range(1, NC * NY):
        hand_on(i).start()
    heads[head] = done[core * NY + tp]
    for i in range(1, NC * NY):
        hand_on(i).wait()
    loads[2].wait()
    attended = jnp.concatenate([heads[i] for i in range(NC * NY)], axis=1)
    mixer_ref[...] = jnp.dot(attended, w_out[...], preferred_element_type=f32).astype(jnp.bfloat16)

    def combine(j, carry):
        each(1, peers, lambda i: give_back(j, i).wait_recv())
        back = returned[j].reshape(peers * returned.shape[2], cols)
        moe_ref[:, pl.ds(pl.multiple_of(j * cols, cols), cols)] = (
            jnp.dot(high[...], back, preferred_element_type=f32)
            + jnp.dot(low[...], back, preferred_element_type=f32)
        ).astype(jnp.bfloat16)
        return carry

    lax.fori_loop(0, parts, combine, 0)

    each(1, peers, lambda i: dispatch(i).wait_send())
    for j in range(parts):
        each(1, peers, lambda i: give_back(j, i).wait_send())
    for side in range(2):
        for step in range(3):
            for n in range(2):
                gate_up(n, step, side).wait_send()
            for j in range(parts):
                down(j, step, side).wait_send()
        for hop in range(1, NZ // 2 + 1):
            along_z(hop, side).wait_send()
        for b in range(NZ):
            for step in range(2):
                along_x(b, step, side).wait_send()


def whole_step(parts, *args):
    q, k, v, lam, gain, w_out, rows, ffn, routes, groups, picks, w_gate, w_up, w_down = args
    bf16, f32 = jnp.bfloat16, jnp.float32
    peers = NZ * NX * NC
    count, width = q.shape[0], rows.shape[1]
    capacity = 8
    tokens = rows.shape[0] // NY
    deep = w_down.shape[0]
    own_rows = count // NY
    dma = lambda n: pltpu.SemaphoreType.DMA((n,))
    return pl.pallas_call(
        functools.partial(step_kernel, parts),
        name="whole_step",
        out_shape=(
            jax.ShapeDtypeStruct((own_rows, width), bf16),
            jax.ShapeDtypeStruct((tokens, width), bf16),
        ),
        in_specs=[ANY, ANY, ANY, VMEM, VMEM, ANY, ANY, VMEM, VMEM, VMEM, VMEM, ANY, ANY, ANY],
        out_specs=(VMEM, VMEM),
        scratch_shapes=[
            pltpu.VMEM((tokens, width), bf16),
            pltpu.VMEM((tokens, peers * capacity), bf16),
            pltpu.VMEM((tokens, peers * capacity), bf16),
            pltpu.VMEM((NY, *w_gate.shape), bf16),
            pltpu.VMEM((NY, *w_up.shape), bf16),
            pltpu.VMEM((parts, NY * deep, width // parts), bf16),
            pltpu.VMEM((peers, capacity, width), bf16),
            pltpu.VMEM((peers, capacity, width), bf16),
            pltpu.VMEM((peers * capacity, NY * deep), bf16),
            pltpu.VMEM((parts, peers, capacity, width // parts), bf16),
            pltpu.VMEM((parts, peers, capacity, width // parts), bf16),
            pltpu.VMEM((2 * count, 128), bf16),
            pltpu.VMEM((4 * count, 128), bf16),
            pltpu.VMEM((peers * count, 256), bf16),
            pltpu.VMEM((4 * count, 1), f32),
            pltpu.VMEM((4 * count, 1), f32),
            pltpu.VMEM((4 * count, 128), f32),
            pltpu.VMEM((NC * NY, own_rows, 128), bf16),
            pltpu.VMEM((NC * NY, own_rows, 128), bf16),
            pltpu.VMEM(w_out.shape, bf16),
            dma(12), dma(12), dma(6 * parts), dma(6 * parts), dma(3), dma(3), dma(NZ), dma(NZ), dma(4 * NZ), dma(4 * NZ),
            dma(peers), dma(peers), dma(parts * peers), dma(parts * peers), dma(NC * NY), dma(NC * NY), dma(7 + parts),
        ],
        compiler_params=pltpu.CompilerParams(has_side_effects=True, vmem_limit_bytes=60 * 2**20),
        cost_estimate=pl.CostEstimate(flops=10**10, bytes_accessed=16 * 2**20, transcendentals=0),
    )(*args)


def local(
    query_rows, key_rows, value_rows, lambdas, head_gain, w_out, moe_rows, ffn_gain,
    routes, group_logits, pick_logits, w_gate, w_up, w_down,
):
    core = lax.axis_index("ep") % NC
    return whole_step(
        4,
        query_rows, key_rows, value_rows, lax.dynamic_slice_in_dim(lambdas, core, 1, 0)[None], head_gain[None], w_out,
        moe_rows, ffn_gain[None], routes, group_logits, pick_logits, w_gate[0], w_up[0], w_down[0],
    )


def solution(mesh):
    return jax.shard_map(
        local,
        mesh=mesh,
        in_specs=(
            P("ep", "tp"), P("ep", "tp"), P("ep", "tp"), P("tp"), P(), P(), P("ep", None), P(), P("ep", None),
            P("ep", None), P("ep", None), P("ep", None, "tp"), P("ep", None, "tp"), P("ep", "tp", None),
        ),
        out_specs=(P(("ep", "tp"), None), P(("ep", "tp"), None)),
        check_vma=False,
    )
```

```python
import jax
import jax.numpy as jnp
from jax import lax
from jax.experimental import pallas as pl
from jax.experimental.pallas import tpu as pltpu
from jax.sharding import PartitionSpec as P

EPS = 1e-06
HEAD_SCALE = 0.8
PIECES = (256, 512, 640, 640)
NZ, NX, NC, NY = 8, 4, 2, 4
ANY = pl.BlockSpec(memory_space=pl.ANY)
VMEM = pl.BlockSpec(memory_space=pltpu.VMEM)
MESH = pl.DeviceIdType.MESH


def plane_peer(ep, i):
    z, x, c = ep // (NX * NC), ep // NC % NX, ep % NC
    k, j = i % NZ, i // NZ
    dz = lax.rem(jnp.where(k % 2 == 1, (k + 1) // 2, NZ - k // 2), NZ)
    dx, dc = j // NC, j % NC
    return (lax.rem(z + dz, NZ) * NX + lax.rem(x + dx, NX)) * NC + lax.rem(c + dc, NC)


def step_kernel(
    q_ref, k_ref, v_ref, lam_ref, gain_ref, w_out_ref, rows_ref, ffn_ref, routes_ref, groups_ref, picks_ref,
    g_ref, u_ref, d_ref, mixer_ref, moe_ref,
    rows_in, high, low, gates, ups, sent, arrived, hidden, queries, spread, kv, top, total, acc, done, heads, w_out,
    g_send, g_recv, d_send, d_recv, p_send, p_recv, z_send, z_recv, x_send, x_recv,
    a_send, a_recv, r_send, r_recv, h_send, h_recv, own_sem, met, *pieces,
):
    parts = len(PIECES)
    starts = [sum(PIECES[:j]) for j in range(parts)]
    downs, results, returned = pieces[:parts], pieces[parts : 2 * parts], pieces[2 * parts :]
    ep, tp = lax.axis_index("ep"), lax.axis_index("tp")
    z, x, core = ep // (NX * NC), ep // NC % NX, ep % NC
    chip = ep // NC
    head = tp * NC + core
    peers = NZ * NX * NC
    f32 = jnp.float32

    def remote(src, dst, send, recv, at, device):
        return pltpu.make_async_remote_copy(
            src_ref=src, dst_ref=dst, send_sem=send.at[at], recv_sem=recv.at[at],
            device_id=device, device_id_type=MESH,
        )

    tp_side = (lax.rem(tp + 1, NY), lax.rem(tp + NY - 1, NY))

    def gate_up(n, step, side):
        src, full = ((g_ref, gates), (u_ref, ups))[n]
        rows = src.shape[0] // 2
        h = (step + side) % 2 if step < 2 else side
        part = pl.ds(h * rows, rows)
        frm = src.at[part] if step < 2 else full.at[1 + side, part]
        to = full.at[1 + side if step < 2 else 3, part]
        return remote(frm, to, g_send, g_recv, (n * 3 + step) * 2 + side, (ep, tp_side[side]))

    def down(j, step, side):
        rows = d_ref.shape[0] // 2
        h = (step + side) % 2 if step < 2 else side
        row = lambda place: pl.ds((place * 2 + h) * rows, rows)
        if step < 2:
            frm = d_ref.at[pl.ds(h * rows, rows), pl.ds(starts[j], PIECES[j])]
            to = downs[j].at[row(1 + side)]
        else:
            frm = downs[j].at[row(1 + side)]
            to = downs[j].at[row(3)]
        return remote(frm, to, d_send, d_recv, (j * 3 + step) * 2 + side, (ep, tp_side[side]))

    both = lambda make: [make(0), make(1)]

    def down_first(j):
        for step in range(2):
            for c in both(lambda side: down(j, step, side)):
                c.start()

    def down_onward(j):
        for side in range(2):
            down(j, 0, side).wait_recv()
            down(j, 2, side).start()

    partner = chip * NC + 1 - core
    next_z = [((lax.rem(z + dz, NZ) * NX + x) * NC + core, tp) for dz in (1, NZ - 1)]
    next_x = [((z * NX + lax.rem(x + dx, NX)) * NC + core, tp) for dx in (1, NX - 1)]
    next_y = [(ep, side) for side in tp_side]
    near = next_z + next_x + next_y + [(partner, tp)]
    barrier = pltpu.get_barrier_semaphore()
    for device in near:
        pl.semaphore_signal(barrier, inc=1, device_id=device, device_id_type=MESH)
    pl.semaphore_wait(barrier, len(near))

    def meet(turn, devices):
        for n, device in enumerate(devices):
            pl.semaphore_signal(met.at[turn * 2 + n], inc=1, device_id=device, device_id_type=MESH)
        for n in range(len(devices)):
            pl.semaphore_wait(met.at[turn * 2 + n], 1)

    for step in range(2):
        for n in range(2):
            for c in both(lambda side: gate_up(n, step, side)):
                c.start()

    mine = pl.ds(pl.multiple_of(core * 128, 128), 128)
    other = pl.ds(pl.multiple_of((1 - core) * 128, 128), 128)
    count = q_ref.shape[0]
    place_of = pl.ds(pl.multiple_of(core * count, count), count)
    kv_rows = pl.ds(pl.multiple_of((chip * NC + core) * count, count), count)
    triples = (
        (q_ref, queries.at[place_of]),
        (k_ref, kv.at[kv_rows, pl.ds(0, 128)]),
        (v_ref, kv.at[kv_rows, pl.ds(128, 128)]),
    )
    swaps = [remote(src.at[:, other], dst, p_send, p_recv, n, (partner, tp)) for n, (src, dst) in enumerate(triples)]
    keeps = [pltpu.make_async_copy(src.at[:, mine], dst, own_sem.at[n]) for n, (src, dst) in enumerate(triples)]
    for c in swaps + keeps:
        c.start()
    deep = d_ref.shape[0]
    loads = [
        pltpu.make_async_copy(g_ref, gates.at[0], own_sem.at[3]),
        pltpu.make_async_copy(u_ref, ups.at[0], own_sem.at[4]),
        pltpu.make_async_copy(w_out_ref, w_out, own_sem.at[5]),
    ] + [
        pltpu.make_async_copy(d_ref.at[:, pl.ds(starts[j], PIECES[j])], downs[j].at[pl.ds(0, deep)], own_sem.at[6 + j])
        for j in range(parts)
    ]
    tokens = rows_in.shape[0]
    load_rows = pltpu.make_async_copy(
        rows_ref.at[pl.ds(pl.multiple_of(tp * tokens, tokens), tokens)], rows_in, own_sem.at[6 + parts]
    )
    for c in [load_rows] + loads:
        c.start()

    chip_rows = kv.shape[0] // (NZ * NX)
    at_z = lambda dz: lax.rem(z + dz + NZ, NZ)
    at_x = lambda dx: lax.rem(x + dx + NX, NX)

    def kv_block(dz, dx, h=None):
        start = (at_z(dz) * NX + at_x(dx)) * chip_rows
        rows = chip_rows
        if h is not None:
            rows = chip_rows // 2
            start = start + h * rows
        return kv.at[pl.ds(pl.multiple_of(start, rows), rows)]

    def along_z(hop, side):
        sign = 1 if side == 0 else -1
        ref = kv_block(-sign * (hop - 1), 0, side if hop == NZ // 2 else None)
        device = ((at_z(sign) * NX + x) * NC + core, tp)
        return remote(ref, ref, z_send, z_recv, (hop - 1) * 2 + side, device)

    blocks = [0, -1, 1, -2, 2, -3, 3, 4]

    def along_x(b, step, side):
        sign = 1 if side == 0 else -1
        ref = kv_block(blocks[b], 0) if step == 0 else kv_block(blocks[b], -sign, side)
        device = ((z * NX + at_x(sign)) * NC + core, tp)
        return remote(ref, ref, x_send, x_recv, (b * 2 + step) * 2 + side, device)

    def x_first(b):
        for c in both(lambda side: along_x(b, 0, side)):
            c.start()

    def x_onward(b):
        for side in range(2):
            along_x(b, 0, side).wait_recv()
            along_x(b, 1, side).start()

    def z_hop(hop):
        for side in range(2):
            along_z(hop, side).wait_recv()
            if hop < NZ // 2:
                along_z(hop + 1, side).start()

    def dispatch(i):
        peer = plane_peer(ep, i)
        return remote(sent.at[peer], arrived.at[ep], a_send, a_recv, i, (peer, tp))

    def give_back(j, i):
        peer = plane_peer(ep, i)
        return remote(results[j].at[peer], returned[j].at[ep], r_send, r_recv, j * peers + i, (peer, tp))

    def each(first, last, act):
        def one(i, carry):
            act(i)
            return carry

        lax.fori_loop(first, last, one, 0)

    load_rows.wait()
    rows = rows_in[...].astype(f32)
    squared = jnp.mean(rows * rows, axis=-1, keepdims=True)
    normed = (rows * lax.rsqrt(squared + EPS) * ffn_ref[...]).astype(jnp.bfloat16)
    own_rows = pl.ds(pl.multiple_of(tp * tokens, tokens), tokens)
    lane = lax.broadcasted_iota(jnp.int32, (tokens, tokens), 1)
    below = lax.broadcasted_iota(jnp.int32, (tokens, tokens), 0)

    def columns(ref):
        rows = ref[:, own_rows].astype(f32)
        turned = [
            jnp.sum(jnp.where(lane == below, rows[k : k + 1], 0.0), axis=-1, keepdims=True) for k in range(ref.shape[0])
        ]
        return jnp.concatenate(turned, axis=1)

    chosen = columns(routes_ref).astype(jnp.int32)
    logits = columns(groups_ref)
    group_weights = jnp.exp(logits - jnp.max(logits, axis=-1, keepdims=True))
    group_weights = group_weights / jnp.sum(group_weights, axis=-1, keepdims=True)
    logits = columns(picks_ref)
    pick_weights = jnp.exp(logits - jnp.max(logits, axis=-1, keepdims=True))
    pick_weights = pick_weights / jnp.sum(pick_weights, axis=-1, keepdims=True)
    earlier = (lane < below).astype(f32).astype(jnp.bfloat16)
    named = [lane == chosen[:, k : k + 1] for k in range(2)]
    either = jnp.where(named[0] | named[1], 1.0, 0.0).astype(jnp.bfloat16)
    before = jnp.dot(earlier, either, preferred_element_type=f32)
    capacity = sent.shape[1]
    every = lax.broadcasted_iota(jnp.int32, (tokens, peers * capacity), 1).astype(f32)
    group_size = peers // groups_ref.shape[0]
    group_lane = lax.broadcasted_iota(jnp.int32, group_weights.shape, 1) * group_size
    place = jnp.zeros((tokens, peers * capacity), f32)
    mixing = jnp.zeros((tokens, peers * capacity), f32)
    for k in range(2):
        expert = chosen[:, k : k + 1]
        rank = jnp.sum(jnp.where(named[k], before, 0.0), axis=-1, keepdims=True)
        hit = every == expert.astype(f32) * capacity + rank
        inside = (expert >= group_lane) & (expert < group_lane + group_size)
        share = jnp.sum(jnp.where(inside, group_weights, 0.0), axis=-1, keepdims=True)
        place = jnp.where(hit, 1.0, place)
        mixing = jnp.where(hit, share * pick_weights[:, k : k + 1], mixing)
    high[...] = mixing.astype(jnp.bfloat16)
    low[...] = (mixing - mixing.astype(jnp.bfloat16).astype(f32)).astype(jnp.bfloat16)
    sent[...] = (
        lax.dot_general(place.astype(jnp.bfloat16), normed, (((0,), (0,)), ((), ())), preferred_element_type=f32)
        .astype(jnp.bfloat16)
        .reshape(sent.shape)
    )
    arrived[ep] = sent[ep]

    for c in keeps:
        c.wait()
    for c in swaps:
        c.wait()
    for c in both(lambda side: along_z(1, side)):
        c.start()
    x_first(0)
    for turn in range(3):
        meet(turn, next_z)
    for turn in range(3, 5):
        meet(turn, next_x)
    meet(5, [(partner, tp)])
    each(1, peers, lambda i: dispatch(i).start())

    scaled = queries[...] * jnp.bfloat16(0.125)
    column = lax.broadcasted_iota(jnp.int32, scaled.shape, 1)
    zero = jnp.zeros_like(scaled)
    spread[0 : 2 * count] = jnp.where(column < 64, scaled, zero)
    spread[2 * count :] = jnp.where(column < 64, zero, scaled)
    top[...] = jnp.full_like(top, -1e30)
    total[...] = jnp.zeros_like(total)
    acc[...] = jnp.zeros_like(acc)

    z_hop(1)
    x_first(1)
    x_first(2)
    for side in range(2):
        gate_up(0, 0, side).wait_recv()
        gate_up(0, 2, side).start()
    down_first(0)
    for side in range(2):
        gate_up(1, 0, side).wait_recv()
        gate_up(1, 2, side).start()
    for b in range(3):
        x_onward(b)

    def absorb(first, last):
        size = NX * chip_rows

        def one(b, carry):
            for side in range(2):
                half = kv.at[pl.ds(0, chip_rows // 2)]
                remote(half, half, x_send, x_recv, (b * 2 + 1) * 2 + side, (partner, tp)).wait_recv()
            dz = jnp.where(b % 2 == 1, NZ - (b + 1) // 2, b // 2)
            absorb_at(pl.ds(pl.multiple_of(lax.rem(z + dz, NZ) * size, size), size))
            return carry

        lax.fori_loop(first, last, one, 0)

    def absorb_at(at):
        scores = lax.dot_general(spread[...], kv[at, 0:128], (((1,), (1,)), ((), ())), preferred_element_type=f32)
        old = top[...]
        new = jnp.maximum(old, jnp.max(scores, axis=-1, keepdims=True))
        factor = jnp.exp(old - new)
        weights = jnp.exp(scores - new)
        total[...] = total[...] * factor + jnp.sum(weights, axis=-1, keepdims=True)
        acc[...] = acc[...] * factor + jnp.dot(
            weights.astype(jnp.bfloat16), kv[at, 128:256], preferred_element_type=f32
        )
        top[...] = new

    for turn in range(6, 8):
        meet(turn, next_y)
    absorb(0, 3)

    each(1, peers, lambda i: dispatch(i).wait_recv())
    for c in loads[:2]:
        c.wait()

    def one_part(s, carry):
        @pl.when(s == 1)
        def _():
            for n in range(2):
                gate_up(n, 1, 0).wait_recv()
            z_hop(2)
            x_first(3)
            x_first(4)

        @pl.when(s == 2)
        def _():
            for n in range(2):
                gate_up(n, 1, 1).wait_recv()

        @pl.when(s == 3)
        def _():
            for n in range(2):
                for side in range(2):
                    gate_up(n, 2, side).wait_recv()

        rows_at = arrived[...].reshape(peers * arrived.shape[1], arrived.shape[2])
        gate = jnp.dot(rows_at, gates[s], preferred_element_type=f32)
        up = jnp.dot(rows_at, ups[s], preferred_element_type=f32)
        hidden[:, pl.ds(pl.multiple_of(s * deep, deep), deep)] = (gate / (1.0 + jnp.exp(-gate)) * up).astype(jnp.bfloat16)
        return carry

    lax.fori_loop(0, NY, one_part, 0)

    def between(j):
        if j == 0:
            down_onward(0)
            down_first(1)
            z_hop(3)
            x_first(5)
            x_first(6)
        elif j == 1:
            down_onward(1)
            down_first(2)
            x_onward(3)
            x_onward(4)
            z_hop(4)
            x_first(7)
        elif j == 2:
            down_onward(2)
            down_first(3)
            x_onward(5)
            x_onward(6)
            absorb(3, 4)
        elif j == 3:
            down_onward(3)
            x_onward(7)
            absorb(4, 5)

    for j in range(parts):
        between(j)
        for side in range(2):
            down(j, 1, side).wait_recv()
            down(j, 2, side).wait_recv()
        loads[3 + j].wait()
        results[j][...] = (
            jnp.dot(hidden[...], downs[j][...], preferred_element_type=f32)
            .astype(jnp.bfloat16)
            .reshape(results[j].shape)
        )
        returned[j][ep] = results[j][ep]
        each(1, peers, lambda i: give_back(j, i).start())
    absorb(5, 8)

    lam = jnp.where(core == 0, lam_ref[:, 0:1], lam_ref[:, 1:2])
    per_head = acc[0 : 2 * count] / total[0 : 2 * count] - lam * (acc[2 * count :] / total[2 * count :])
    squared = jnp.mean(per_head * per_head, axis=-1, keepdims=True)
    normed = per_head * lax.rsqrt(squared + EPS) * gain_ref[...] * HEAD_SCALE
    done[...] = normed.astype(jnp.bfloat16).reshape(done.shape)

    def hand_on(i):
        to_core = lax.rem(core + i // NY, NC)
        to_tp = lax.rem(tp + i % NY, NY)
        return remote(
            done.at[to_core * NY + to_tp], heads.at[head], h_send, h_recv, i, (chip * NC + to_core, to_tp)
        )

    for i in range(1, NC * NY):
        hand_on(i).start()
    heads[head] = done[core * NY + tp]
    for i in range(1, NC * NY):
        hand_on(i).wait()
    loads[2].wait()
    attended = jnp.concatenate([heads[i] for i in range(NC * NY)], axis=1)
    mixer_ref[...] = jnp.dot(attended, w_out[...], preferred_element_type=f32).astype(jnp.bfloat16)

    for j in range(parts):
        each(1, peers, lambda i: give_back(j, i).wait_recv())
        back = returned[j][...].reshape(peers * capacity, PIECES[j])
        moe_ref[:, starts[j] : starts[j] + PIECES[j]] = (
            jnp.dot(high[...], back, preferred_element_type=f32) + jnp.dot(low[...], back, preferred_element_type=f32)
        ).astype(jnp.bfloat16)

    each(1, peers, lambda i: dispatch(i).wait_send())
    for j in range(parts):
        each(1, peers, lambda i: give_back(j, i).wait_send())
    for side in range(2):
        for step in range(3):
            for n in range(2):
                gate_up(n, step, side).wait_send()
            for j in range(parts):
                down(j, step, side).wait_send()
        for hop in range(1, NZ // 2 + 1):
            along_z(hop, side).wait_send()
        for b in range(NZ):
            for step in range(2):
                along_x(b, step, side).wait_send()


def whole_step(*args):
    q, k, v, lam, gain, w_out, rows, ffn, routes, groups, picks, w_gate, w_up, w_down = args
    bf16, f32 = jnp.bfloat16, jnp.float32
    peers = NZ * NX * NC
    count, width = q.shape[0], rows.shape[1]
    capacity = 8
    tokens = rows.shape[0] // NY
    deep = w_down.shape[0]
    own_rows = count // NY
    parts = len(PIECES)
    dma = lambda n: pltpu.SemaphoreType.DMA((n,))
    return pl.pallas_call(
        step_kernel,
        name="whole_step",
        out_shape=(
            jax.ShapeDtypeStruct((own_rows, width), bf16),
            jax.ShapeDtypeStruct((tokens, width), bf16),
        ),
        in_specs=[ANY, ANY, ANY, VMEM, VMEM, ANY, ANY, VMEM, VMEM, VMEM, VMEM, ANY, ANY, ANY],
        out_specs=(VMEM, VMEM),
        scratch_shapes=[
            pltpu.VMEM((tokens, width), bf16),
            pltpu.VMEM((tokens, peers * capacity), bf16),
            pltpu.VMEM((tokens, peers * capacity), bf16),
            pltpu.VMEM((NY, *w_gate.shape), bf16),
            pltpu.VMEM((NY, *w_up.shape), bf16),
            pltpu.VMEM((peers, capacity, width), bf16),
            pltpu.VMEM((peers, capacity, width), bf16),
            pltpu.VMEM((peers * capacity, NY * deep), bf16),
            pltpu.VMEM((2 * count, 128), bf16),
            pltpu.VMEM((4 * count, 128), bf16),
            pltpu.VMEM((peers * count, 256), bf16),
            pltpu.VMEM((4 * count, 1), f32),
            pltpu.VMEM((4 * count, 1), f32),
            pltpu.VMEM((4 * count, 128), f32),
            pltpu.VMEM((NC * NY, own_rows, 128), bf16),
            pltpu.VMEM((NC * NY, own_rows, 128), bf16),
            pltpu.VMEM(w_out.shape, bf16),
            dma(12), dma(12), dma(6 * parts), dma(6 * parts), dma(3), dma(3), dma(NZ), dma(NZ), dma(4 * NZ), dma(4 * NZ),
            dma(peers), dma(peers), dma(parts * peers), dma(parts * peers), dma(NC * NY), dma(NC * NY), dma(7 + parts),
            pltpu.SemaphoreType.REGULAR((16,)),
        ]
        + [pltpu.VMEM((NY * deep, cols), bf16) for cols in PIECES]
        + [pltpu.VMEM((peers, capacity, cols), bf16) for cols in PIECES * 2],
        compiler_params=pltpu.CompilerParams(collective_id=0, has_side_effects=True, vmem_limit_bytes=60 * 2**20),
        cost_estimate=pl.CostEstimate(flops=10**10, bytes_accessed=16 * 2**20, transcendentals=0),
    )(*args)


def local(
    query_rows, key_rows, value_rows, lambdas, head_gain, w_out, moe_rows, ffn_gain,
    routes, group_logits, pick_logits, w_gate, w_up, w_down,
):
    return whole_step(
        query_rows, key_rows, value_rows, lambdas[None], head_gain[None], w_out,
        moe_rows, ffn_gain[None], routes.T, group_logits.T, pick_logits.T, w_gate[0], w_up[0], w_down[0],
    )


def solution(mesh):
    return jax.shard_map(
        local,
        mesh=mesh,
        in_specs=(
            P("ep", "tp"), P("ep", "tp"), P("ep", "tp"), P("tp"), P(), P(), P("ep", None), P(), P("ep", None),
            P("ep", None), P("ep", None), P("ep", None, "tp"), P("ep", None, "tp"), P("ep", "tp", None),
        ),
        out_specs=(P(("ep", "tp"), None), P(("ep", "tp"), None)),
        check_vma=False,
    )
```
